32 devices in a mesh: kv: 16 (over z, y, x), tp: 2 (over core).
Axes of the slice: x: 2, y: 2, z: 4, core: 2. Of those that a mesh axis runs over, the one named last changes fastest.
Arguments:
- tokens: bfloat16 [64, 4, 2048], P('kv', None, 'tp'), may hold values from -6 to 6
- input_gain: float32 [2048], replicated, may hold values from 0.1 to 1.9
- gate_weight: bfloat16 [2048, 4096], P('kv', 'tp'), may hold values from -0.125 to 0.125
- value_weight: bfloat16 [2048, 4096], P('kv', 'tp'), may hold values from -0.125 to 0.125
- write_weight: bfloat16 [2048, 1024], P('kv', 'tp'), may hold values from -0.125 to 0.125
- read_weight: bfloat16 [2048, 1024], P('kv', 'tp'), may hold values from -0.125 to 0.125
- step_weight: bfloat16 [2048, 64], replicated, may hold values from -0.125 to 0.125
- conv_value: float32 [4, 4096], P(None, 'tp'), may hold values from -3 to 3
- conv_write: float32 [4, 1024], P(None, 'tp'), may hold values from -3 to 3
- conv_read: float32 [4, 1024], P(None, 'tp'), may hold values from -3 to 3
- step_bias: float32 [64], P('tp'), may hold values from -4 to -1
- decay_log: float32 [64], P('tp'), may hold values from 0 to 2.8
- skip_gain: float32 [64], P('tp'), may hold values from 0.5 to 1.5
- output_gain: float32 [4096], P('tp'), may hold values from 0.1 to 1.9
- out_weight: bfloat16 [4096, 2048], P('tp', 'kv'), may hold values from -0.09375 to 0.09375
- base_state: float32 [64, 64, 64, 128], P('kv', 'tp'), may hold values from -2 to 2
- past_value: bfloat16 [64, 7, 4096], P('kv', None, 'tp'), may hold values from -6 to 6
- past_write: bfloat16 [64, 7, 1024], P('kv', None, 'tp'), may hold values from -6 to 6
- past_read: bfloat16 [64, 7, 1024], P('kv', None, 'tp'), may hold values from -6 to 6
- past_step: bfloat16 [64, 4, 64], P('kv', None, 'tp'), may hold values from -4 to 4
- accepted: int32 [64], P('kv'), may hold values from 1 to 4
Outputs:
- mixed: bfloat16 [64, 4, 2048], P('kv', None, 'tp')
- root_state: float32 [64, 64, 64, 128], P('kv', 'tp')
- next_value: bfloat16 [64, 7, 4096], P('kv', None, 'tp')
- next_write: bfloat16 [64, 7, 1024], P('kv', None, 'tp')
- next_read: bfloat16 [64, 7, 1024], P('kv', None, 'tp')
- next_step: bfloat16 [64, 4, 64], P('kv', None, 'tp')
The draws below stay inside these ranges and needn't reach their ends.
Inputs may be any that keep to these rules, and one draw needn't show every extreme that they name: Every entry of `accepted` is an integer from 1 to 4 (at least one of the last step's proposals is always accepted).
All inputs are finite; a program needn't handle non-finite values.
Results may differ from the reference program's by a relative error of at most 0.018.
Values may be sent and summed in bfloat16 or wider, within the bound.
A program may use at most 64 MiB of HBM per device.

```python
import jax
import jax.numpy as jnp
from jax import lax

WIDTH = 2048
INNER = 4096
HEADS = 64
HEAD_DIM = 64
GROUPS = 8
STATE_DIM = 128
CONV_W = 4
PROPOSALS = 4
SEQS = 64
PAST_ROWS = 7
N_TP = 2


def plant(entries, key, smallest, high):
    dims = entries.shape
    spot = [jax.random.randint(jax.random.fold_in(key, axis), (), 0, dims[axis]) for axis in range(len(dims))]
    entries = entries.at[tuple(spot)].set(smallest)
    longest = dims.index(max(dims))
    spot[longest] = (spot[longest] + 1) % dims[longest]
    return entries.at[tuple(spot)].set(high)


def levels(stream_key, shape, pieces, low, high):
    level = 1.0
    for dim, parts in pieces:
        draws = jax.random.uniform(jax.random.fold_in(jax.random.fold_in(stream_key, 6), dim), (parts,), jnp.float32, low / len(pieces), high / len(pieces))
        level = level * jnp.repeat(jnp.exp(draws), shape[dim] // parts).reshape((-1,) + (1,) * (len(shape) - 1 - dim))
    return level


def noise(key, extent, scale, most, shards=(), kind=jnp.bfloat16):
    loudness = levels(key, extent, shards, -0.22, 0.18) if shards else 1.0
    values = jax.random.normal(key, extent, jnp.float32) * scale * loudness
    return jnp.minimum(jnp.maximum(values, -most), most).astype(kind)


def setup_inputs(seed: int = 0) -> dict:
    key_of = jax.random.split(jax.random.key(seed), 22)
    tokens = noise(key_of[0], (SEQS, PROPOSALS, WIDTH), 1.0, 6.0, ((0, 16), (2, 2)))
    input_gain = jnp.clip(1.0 + 0.18 * jax.random.normal(key_of[1], (WIDTH,), jnp.float32), 0.1, 1.9)
    gate_weight = noise(key_of[2], (WIDTH, INNER), WIDTH ** -0.5, 0.125, ((0, 16), (1, 2)))
    value_weight = noise(key_of[3], (WIDTH, INNER), WIDTH ** -0.5, 0.125, ((0, 16), (1, 2)))
    write_weight = noise(key_of[4], (WIDTH, GROUPS * STATE_DIM), WIDTH ** -0.5, 0.125, ((0, 16), (1, 2)))
    read_weight = noise(key_of[5], (WIDTH, GROUPS * STATE_DIM), WIDTH ** -0.5, 0.125, ((0, 16), (1, 2)))
    step_weight = noise(key_of[6], (WIDTH, HEADS), WIDTH ** -0.5, 0.125)
    conv_value = noise(key_of[7], (CONV_W, INNER), 0.5, 3.0, ((1, 2),), jnp.float32)
    conv_write = noise(key_of[8], (CONV_W, GROUPS * STATE_DIM), 0.5, 3.0, ((1, 2),), jnp.float32)
    conv_read = noise(key_of[9], (CONV_W, GROUPS * STATE_DIM), 0.5, 3.0, ((1, 2),), jnp.float32)
    step_bias = jnp.clip(-4.0 + 3.0 * jax.random.uniform(key_of[10], (HEADS,), jnp.float32) ** levels(key_of[10], (HEADS,), ((0, 2),), -0.2, 0.2), -4.0, -1.0)
    decay_log = jnp.clip(2.8 * jax.random.uniform(key_of[11], (HEADS,), jnp.float32) ** levels(key_of[11], (HEADS,), ((0, 2),), -0.2, 0.2), 0.0, 2.8)
    skip_gain = jnp.clip(0.5 + 1.0 * jax.random.uniform(key_of[12], (HEADS,), jnp.float32) ** levels(key_of[12], (HEADS,), ((0, 2),), -0.2, 0.2), 0.5, 1.5)
    output_gain = jnp.clip(1.0 + 0.18 * jax.random.normal(key_of[13], (INNER,), jnp.float32), 0.1, 1.9)
    out_weight = noise(key_of[14], (INNER, WIDTH), INNER ** -0.5, 0.09375, ((0, 2), (1, 16)))
    base_state = noise(key_of[15], (SEQS, HEADS, HEAD_DIM, STATE_DIM), 0.3, 2.0, ((0, 16), (1, 2)), jnp.float32)
    past_value = noise(key_of[16], (SEQS, PAST_ROWS, INNER), 1.0, 6.0, ((0, 16), (2, 2)))
    past_write = noise(key_of[17], (SEQS, PAST_ROWS, GROUPS * STATE_DIM), 1.0, 6.0, ((0, 16), (2, 2)))
    past_read = noise(key_of[18], (SEQS, PAST_ROWS, GROUPS * STATE_DIM), 1.0, 6.0, ((0, 16), (2, 2)))
    past_step = noise(key_of[19], (SEQS, PROPOSALS, HEADS), 1.0, 4.0, ((0, 16), (2, 2)))
    accepted = plant(jax.random.randint(key_of[20], (SEQS,), 1, PROPOSALS + 1), jax.random.fold_in(key_of[20], 1), 1, PROPOSALS).astype(jnp.int32)
    return dict(tokens=tokens, input_gain=input_gain, gate_weight=gate_weight, value_weight=value_weight, write_weight=write_weight, read_weight=read_weight, step_weight=step_weight, conv_value=conv_value, conv_write=conv_write, conv_read=conv_read, step_bias=step_bias, decay_log=decay_log, skip_gain=skip_gain, output_gain=output_gain, out_weight=out_weight, base_state=base_state, past_value=past_value, past_write=past_write, past_read=past_read, past_step=past_step, accepted=accepted)


EPSILON = 1e-06

def causal_conv(rows, kernel):
    width = kernel.shape[0]
    count = rows.shape[0] - width + 1
    total = kernel[0] * rows[0:count]
    for offset in range(1, width):
        total = total + kernel[offset] * rows[offset:offset + count]
    return total

def advance(past_x, past_b, past_c, past_dt, taken, state_zero, value_now, write_now, read_now, gate_now, step_now, conv_value, conv_write, conv_read, step_bias, decay_log, skip_gain, output_gain):
    highest = lax.Precision.HIGHEST
    proposals = value_now.shape[0]
    head_count = step_bias.shape[0]
    group_count = write_now.shape[1] // STATE_DIM
    per_group = head_count // group_count
    head_width = value_now.shape[1] // head_count
    rate = jnp.exp(decay_log)
    taken = taken.astype(jnp.int32)
    prev_x = jax.nn.silu(causal_conv(past_x.astype(jnp.float32), conv_value)).reshape(proposals, head_count, head_width)
    prev_b = jax.nn.silu(causal_conv(past_b.astype(jnp.float32), conv_write)).reshape(proposals, group_count, STATE_DIM)
    prev_b = jnp.repeat(prev_b, per_group, axis=1)
    prev_dt = jax.nn.softplus(past_dt.astype(jnp.float32) + step_bias)
    live = (jnp.arange(proposals, dtype=jnp.int32) < taken)[:, None]
    prev_log = jnp.where(live, -rate * prev_dt, jnp.zeros_like(prev_dt))
    total_log = lax.optimization_barrier(jnp.sum(prev_log, axis=0))
    tail_log = total_log - jnp.cumsum(prev_log, axis=0)
    weight_now = jnp.where(live, jnp.exp(tail_log) * prev_dt, jnp.zeros_like(prev_dt))
    root = jnp.exp(total_log)[:, None, None] * state_zero + jnp.einsum('sh,shp,shn->hpn', weight_now, prev_x, prev_b, precision=highest)
    window_x = jnp.concatenate([lax.dynamic_slice_in_dim(past_x, taken, CONV_W - 1, 0), value_now], axis=0)
    window_b = jnp.concatenate([lax.dynamic_slice_in_dim(past_b, taken, CONV_W - 1, 0), write_now], axis=0)
    window_c = jnp.concatenate([lax.dynamic_slice_in_dim(past_c, taken, CONV_W - 1, 0), read_now], axis=0)
    cur_x = jax.nn.silu(causal_conv(window_x.astype(jnp.float32), conv_value)).reshape(proposals, head_count, head_width)
    cur_b = jax.nn.silu(causal_conv(window_b.astype(jnp.float32), conv_write)).reshape(proposals, group_count, STATE_DIM)
    cur_c = jax.nn.silu(causal_conv(window_c.astype(jnp.float32), conv_read)).reshape(proposals, group_count, STATE_DIM)
    cur_b = jnp.repeat(cur_b, per_group, axis=1)
    cur_c = jnp.repeat(cur_c, per_group, axis=1)
    cur_dt = jax.nn.softplus(step_now.astype(jnp.float32) + step_bias)
    logs = jnp.cumsum(-rate * cur_dt, axis=0)
    carried = jnp.einsum('thn,hpn->thp', cur_c, root, precision=highest) * jnp.exp(logs)[:, :, None]
    lower = (jnp.arange(proposals)[:, None] >= jnp.arange(proposals)[None, :])[:, :, None]
    diff = logs[:, None, :] - logs[None, :, :]
    decay = jnp.where(lower, jnp.exp(jnp.where(lower, diff, jnp.zeros_like(diff))), jnp.zeros_like(diff))
    scores = jnp.einsum('thn,shn->tsh', cur_c, cur_b, precision=highest) * decay * cur_dt[None, :, :]
    inner = jnp.einsum('tsh,shp->thp', scores, cur_x, precision=highest)
    mixed = carried + inner + skip_gain[None, :, None] * cur_x
    gated = mixed.reshape(proposals, -1) * jax.nn.silu(gate_now.astype(jnp.float32))
    grouped = gated.reshape(proposals, group_count, -1)
    grouped = grouped * lax.rsqrt(lax.optimization_barrier(jnp.mean(grouped * grouped, axis=-1, keepdims=True)) + EPSILON)
    result = (grouped.reshape(proposals, -1) * output_gain).astype(jnp.bfloat16)
    return (result, root, window_x, window_b, window_c)

def reference(tokens, input_gain, gate_weight, value_weight, write_weight, read_weight, step_weight, conv_value, conv_write, conv_read, step_bias, decay_log, skip_gain, output_gain, out_weight, base_state, past_value, past_write, past_read, past_step, accepted):
    seq_count, proposals, width = tokens.shape
    rows = tokens.astype(jnp.float32)
    normed = (rows * lax.rsqrt(lax.optimization_barrier(jnp.mean(rows * rows, axis=-1, keepdims=True)) + EPSILON) * input_gain).astype(jnp.bfloat16)
    flat = normed.reshape(seq_count * proposals, width)

    def project(weight):
        product = jnp.dot(flat, weight, preferred_element_type=jnp.float32).astype(jnp.bfloat16)
        return product.reshape(seq_count, proposals, weight.shape[1])
    gate_now = project(gate_weight)
    value_now = project(value_weight)
    write_now = project(write_weight)
    read_now = project(read_weight)
    step_now = project(step_weight)

    def one_sequence(items):
        return advance(*items, conv_value, conv_write, conv_read, step_bias, decay_log, skip_gain, output_gain)
    normal_out, root_state, next_value, next_write, next_read = lax.map(one_sequence, (past_value, past_write, past_read, past_step, accepted, base_state, value_now, write_now, read_now, gate_now, step_now))
    flat_y = normal_out.reshape(seq_count * proposals, -1)
    block = flat_y.shape[1] // N_TP
    total = jnp.zeros((seq_count * proposals, width), jnp.float32)
    for portion in range(N_TP):
        partial_sum = jnp.dot(flat_y[:, portion * block:(portion + 1) * block], out_weight[portion * block:(portion + 1) * block], preferred_element_type=jnp.float32)
        total = total + lax.optimization_barrier(partial_sum.astype(jnp.bfloat16)).astype(jnp.float32)
    mixed = total.astype(jnp.bfloat16).reshape(seq_count, proposals, width)
    return (mixed, root_state, next_value, next_write, next_read, step_now)
```

```python
import functools

import jax
import jax.numpy as jnp
from jax import lax
from jax.experimental import pallas as pl
from jax.experimental.pallas import tpu as pltpu
from jax.sharding import PartitionSpec as P

STATE_DIM = 128
CONV_W = 4


EPSILON = 1e-06


def causal_conv(rows, kernel):
    width = kernel.shape[0]
    count = rows.shape[0] - width + 1
    total = kernel[0] * rows[0:count]
    for offset in range(1, width):
        total = total + kernel[offset] * rows[offset : offset + count]
    return total


def advance(
    past_x,
    past_b,
    past_c,
    past_dt,
    taken,
    state_zero,
    value_now,
    write_now,
    read_now,
    gate_now,
    step_now,
    conv_value,
    conv_write,
    conv_read,
    step_bias,
    decay_log,
    skip_gain,
    output_gain,
):
    highest = lax.Precision.HIGHEST
    proposals = value_now.shape[0]
    head_count = step_bias.shape[0]
    group_count = write_now.shape[1] // STATE_DIM
    per_group = head_count // group_count
    head_width = value_now.shape[1] // head_count
    rate = jnp.exp(decay_log)
    prev_x = jax.nn.silu(causal_conv(past_x.astype(jnp.float32), conv_value)).reshape(
        proposals, head_count, head_width
    )
    prev_b = jax.nn.silu(causal_conv(past_b.astype(jnp.float32), conv_write)).reshape(
        proposals, group_count, STATE_DIM
    )
    prev_b = jnp.repeat(prev_b, per_group, axis=1)
    prev_dt = jax.nn.softplus(past_dt.astype(jnp.float32) + step_bias)
    live = (jnp.arange(proposals, dtype=jnp.int32) < taken)[:, None]
    prev_log = jnp.where(live, -rate * prev_dt, jnp.zeros_like(prev_dt))
    total_log = jnp.sum(prev_log, axis=0)
    tail_log = total_log - jnp.cumsum(prev_log, axis=0)
    weight_now = jnp.where(live, jnp.exp(tail_log) * prev_dt, jnp.zeros_like(prev_dt))
    root = jnp.exp(total_log)[:, None, None] * state_zero + jnp.einsum(
        "sh,shp,shn->hpn", weight_now, prev_x, prev_b, precision=highest
    )
    window_x = jnp.concatenate(
        [lax.dynamic_slice_in_dim(past_x, taken, CONV_W - 1, 0), value_now], axis=0
    )
    window_b = jnp.concatenate(
        [lax.dynamic_slice_in_dim(past_b, taken, CONV_W - 1, 0), write_now], axis=0
    )
    window_c = jnp.concatenate(
        [lax.dynamic_slice_in_dim(past_c, taken, CONV_W - 1, 0), read_now], axis=0
    )
    cur_x = jax.nn.silu(causal_conv(window_x.astype(jnp.float32), conv_value)).reshape(
        proposals, head_count, head_width
    )
    cur_b = jax.nn.silu(causal_conv(window_b.astype(jnp.float32), conv_write)).reshape(
        proposals, group_count, STATE_DIM
    )
    cur_c = jax.nn.silu(causal_conv(window_c.astype(jnp.float32), conv_read)).reshape(
        proposals, group_count, STATE_DIM
    )
    cur_b = jnp.repeat(cur_b, per_group, axis=1)
    cur_c = jnp.repeat(cur_c, per_group, axis=1)
    cur_dt = jax.nn.softplus(step_now.astype(jnp.float32) + step_bias)
    logs = jnp.cumsum(-rate * cur_dt, axis=0)
    carried = jnp.einsum("thn,hpn->thp", cur_c, root, precision=highest) * jnp.exp(logs)[:, :, None]
    lower = (jnp.arange(proposals)[:, None] >= jnp.arange(proposals)[None, :])[:, :, None]
    diff = logs[:, None, :] - logs[None, :, :]
    decay = jnp.where(
        lower, jnp.exp(jnp.where(lower, diff, jnp.zeros_like(diff))), jnp.zeros_like(diff)
    )
    scores = (
        jnp.einsum("thn,shn->tsh", cur_c, cur_b, precision=highest) * decay * cur_dt[None, :, :]
    )
    inner = jnp.einsum("tsh,shp->thp", scores, cur_x, precision=highest)
    mixed = carried + inner + skip_gain[None, :, None] * cur_x
    gated = mixed.reshape(proposals, -1) * jax.nn.silu(gate_now.astype(jnp.float32))
    grouped = gated.reshape(proposals, group_count, -1)
    grouped = grouped * lax.rsqrt(jnp.mean(grouped * grouped, axis=-1, keepdims=True) + EPSILON)
    result = (grouped.reshape(proposals, -1) * output_gain).astype(jnp.bfloat16)
    return (result, root, window_x, window_b, window_c)


MESH = pl.DeviceIdType.MESH


def near_split(count):
    low = max(d for d in range(1, count + 1) if count % d == 0 and d * d <= count)
    return count // low, low


def remote(src, dst, send, recv, kv, tp):
    return pltpu.make_async_remote_copy(
        src_ref=src,
        dst_ref=dst,
        send_sem=send,
        recv_sem=recv,
        device_id={"kv": kv, "tp": tp},
        device_id_type=MESH,
    )


class Gather:
    def __init__(self, own, slots, send, recv, n_kv):
        self.own, self.slots, self.send, self.recv = own, slots, send, recv
        self.far, self.near = near_split(n_kv)
        self.me, self.tp = lax.axis_index("kv"), lax.axis_index("tp")
        self.h, self.l = lax.div(self.me, self.near), lax.rem(self.me, self.near)
        self.copies = []

    def start(self, src, block, kv):
        copy = remote(
            src,
            self.slots.at[block],
            self.send.at[len(self.copies)],
            self.recv.at[block],
            kv,
            self.tp,
        )
        copy.start()
        self.copies.append(copy)

    def arrive(self, block):
        remote(
            self.own, self.slots.at[block], self.send.at[0], self.recv.at[block], self.me, self.tp
        ).wait_recv()

    def first(self):
        for step in range(1, self.far):
            self.start(self.own, self.me, lax.rem(self.h + step, self.far) * self.near + self.l)
        for step in range(1, self.near):
            self.start(self.own, self.me, self.h * self.near + lax.rem(self.l + step, self.near))

    def relay(self):
        for step in range(1, self.far):
            block = lax.rem(self.h + self.far - step, self.far) * self.near + self.l
            self.arrive(block)
            for side in range(1, self.near):
                self.start(
                    self.slots.at[block],
                    block,
                    self.h * self.near + lax.rem(self.l + side, self.near),
                )

    def finish(self):
        for side in range(1, self.near):
            l = lax.rem(self.l + self.near - side, self.near)
            for step in range(self.far):
                self.arrive(lax.rem(self.h + self.far - step, self.far) * self.near + l)

    def drain(self):
        for copy in self.copies:
            copy.wait_send()


def project_kernel(
    n_kv, n_tp, x_ref, wide_ref, thin_ref, out_ref,
    xs, wides, thins, mine, back,
    x_send, x_recv, tp_send, tp_recv, wide_send, wide_recv, thin_send, thin_recv,
    back_send, back_recv, local_sem,
):
    me, tp = lax.axis_index("kv"), lax.axis_index("tp")
    barrier = pltpu.get_barrier_semaphore()
    for step in range(1, n_kv):
        pl.semaphore_signal(
            barrier, inc=1, device_id={"kv": lax.rem(me + step, n_kv), "tp": tp}, device_id_type=MESH
        )
    for step in range(1, n_tp):
        pl.semaphore_signal(
            barrier, inc=1, device_id={"kv": me, "tp": lax.rem(tp + step, n_tp)}, device_id_type=MESH
        )
    own = [
        pltpu.make_async_copy(x_ref, xs.at[tp, me], local_sem.at[0]),
        pltpu.make_async_copy(wide_ref.at[me], wides.at[me], local_sem.at[1]),
        pltpu.make_async_copy(thin_ref.at[me], thins.at[me], local_sem.at[2]),
    ]
    for copy in own:
        copy.start()
    pl.semaphore_wait(barrier, n_kv - 1 + n_tp - 1)

    gather = Gather(x_ref, xs.at[tp], x_send, x_recv, n_kv)
    gather.first()
    sends = []

    def send_weights(lo, hi):
        for step in range(lo, hi):
            peer = lax.rem(me + step, n_kv)
            for src, dst, ss, rs in (
                (wide_ref, wides, wide_send, wide_recv),
                (thin_ref, thins, thin_send, thin_recv),
            ):
                copy = remote(src.at[peer], dst.at[me], ss.at[step - 1], rs.at[step - 1], peer, tp)
                copy.start()
                sends.append(copy)

    cut = 1 + n_kv // 4
    send_weights(1, cut)
    gather.relay()
    send_weights(cut, n_kv)
    gather.finish()
    for copy in own:
        copy.wait()
    shares = []
    for step in range(1, n_tp):
        copy = remote(
            xs.at[tp], xs.at[tp], tp_send.at[step - 1], tp_recv.at[step - 1],
            me, lax.rem(tp + step, n_tp),
        )
        copy.start()
        shares.append(copy)
    for copy in shares:
        copy.wait_recv()
    for copy in sends:
        copy.wait_recv()

    tokens = x_ref.shape[0]
    half = x_ref.shape[1]
    depth = wide_ref.shape[1]
    per = n_kv // n_tp
    wide_sum = None
    thin_sum = None
    for t in range(n_tp):
        rows = xs[t].reshape(n_kv * tokens, half)
        block = wides[t * per : (t + 1) * per].reshape(half, wide_ref.shape[2])
        term = jnp.dot(rows, block, preferred_element_type=jnp.float32)
        wide_sum = term if wide_sum is None else wide_sum + term
        for k in range(per):
            term = lax.dot_general(
                rows[:, k * depth : (k + 1) * depth],
                thins[t * per + k],
                (((1,), (1,)), ((), ())),
                preferred_element_type=jnp.float32,
            )
            thin_sum = term if thin_sum is None else thin_sum + term
    wide_cols = wide_ref.shape[2]
    cols = mine.shape[2]
    mine[:, :, 0:wide_cols] = wide_sum.astype(jnp.bfloat16).reshape(n_kv, tokens, wide_cols)
    mine[:, :, wide_cols:cols] = thin_sum.astype(jnp.bfloat16).reshape(
        n_kv, tokens, cols - wide_cols
    )
    returns = []
    for step in range(1, n_kv):
        peer = lax.rem(me + step, n_kv)
        copy = remote(
            mine.at[peer], back.at[me], back_send.at[step - 1], back_recv.at[step - 1], peer, tp
        )
        copy.start()
        returns.append(copy)
    out_ref[me] = mine[me]
    gather.drain()
    for copy in shares + sends:
        copy.wait_send()
    for step, copy in enumerate(returns, 1):
        copy.wait_recv()
        source = lax.rem(me + n_kv - step, n_kv)
        out_ref[source] = back[source]
    for copy in returns:
        copy.wait_send()


def project(x, wide, thin, n_kv, n_tp):
    tokens, half = x.shape
    cols = wide.shape[2] + thin.shape[1]
    dma = pltpu.SemaphoreType.DMA
    far, near = near_split(n_kv)
    count = far - 1 + (near - 1) * far
    peers = (max(n_kv - 1, 1),)
    return pl.pallas_call(
        functools.partial(project_kernel, n_kv, n_tp),
        out_shape=jax.ShapeDtypeStruct((n_kv, tokens, cols), jnp.bfloat16),
        in_specs=[pl.BlockSpec(memory_space=pltpu.VMEM)] * 3,
        out_specs=pl.BlockSpec(memory_space=pltpu.VMEM),
        scratch_shapes=[
            pltpu.VMEM((n_tp, n_kv, tokens, half), jnp.bfloat16),
            pltpu.VMEM(wide.shape, jnp.bfloat16),
            pltpu.VMEM(thin.shape, jnp.bfloat16),
            pltpu.VMEM((n_kv, tokens, cols), jnp.bfloat16),
            pltpu.VMEM((n_kv, tokens, cols), jnp.bfloat16),
            dma((count,)), dma((n_kv,)), dma((max(n_tp - 1, 1),)), dma((max(n_tp - 1, 1),)),
            dma(peers), dma(peers), dma(peers), dma(peers), dma(peers), dma(peers), dma((3,)),
        ],
        compiler_params=pltpu.CompilerParams(collective_id=0, has_side_effects=True),
        name="project",
    )(x, wide, thin)


def mix_kernel(
    n_kv, n_tp, y_ref, w_ref, out_ref,
    ys, mine, parts, y_send, y_recv, part_send, part_recv, local_sem,
):
    me, tp = lax.axis_index("kv"), lax.axis_index("tp")
    total = n_kv * n_tp
    flat = me * n_tp + tp
    barrier = pltpu.get_barrier_semaphore()

    def greet(step, carry):
        other = lax.rem(flat + step, total)
        pl.semaphore_signal(
            barrier,
            inc=1,
            device_id={"kv": lax.div(other, n_tp), "tp": lax.rem(other, n_tp)},
            device_id_type=MESH,
        )
        return carry

    lax.fori_loop(1, total, greet, 0)
    own = pltpu.make_async_copy(y_ref, ys.at[me], local_sem.at[0])
    own.start()
    pl.semaphore_wait(barrier, total - 1)
    gather = Gather(y_ref, ys, y_send, y_recv, n_kv)
    gather.first()
    gather.relay()
    own.wait()
    gather.finish()

    tokens, cols = y_ref.shape[0], w_ref.shape[1]
    product = jnp.dot(
        ys[...].reshape(n_kv * tokens, y_ref.shape[1]),
        w_ref[...],
        preferred_element_type=jnp.float32,
    )
    mine[...] = product.astype(jnp.bfloat16).reshape(n_kv, tokens, cols)
    per = n_kv // n_tp
    side, place = lax.div(me, per), lax.rem(me, per)

    def part(step):
        return remote(
            mine.at[lax.rem(me + step, n_kv)],
            parts.at[tp, place],
            part_send.at[step],
            part_recv.at[tp, place],
            lax.rem(me + step, n_kv),
            side,
        )

    for step in range(1, n_kv):
        part(step).start()

    @pl.when(side != tp)
    def _():
        part(0).start()

    @pl.when(side == tp)
    def _():
        parts[tp, place] = mine[me]

    gather.drain()
    for t in range(n_tp):
        for k in range(per):
            incoming = remote(
                mine.at[0], parts.at[t, k], part_send.at[0], part_recv.at[t, k], me, tp
            )

            @pl.when(jnp.logical_or(t != tp, tp * per + k != me))
            def _():
                incoming.wait_recv()

    for k in range(per):
        value = parts[0, k].astype(jnp.float32)
        for t in range(1, n_tp):
            value = value + parts[t, k].astype(jnp.float32)
        out_ref[:, k * cols : (k + 1) * cols] = value.astype(jnp.bfloat16)
    for step in range(1, n_kv):
        part(step).wait_send()

    @pl.when(side != tp)
    def _():
        part(0).wait_send()


def mix(y, weight, n_kv, n_tp):
    tokens, depth = y.shape
    cols = weight.shape[1]
    dma = pltpu.SemaphoreType.DMA
    far, near = near_split(n_kv)
    count = far - 1 + (near - 1) * far
    per = n_kv // n_tp
    return pl.pallas_call(
        functools.partial(mix_kernel, n_kv, n_tp),
        out_shape=jax.ShapeDtypeStruct((tokens, per * cols), jnp.bfloat16),
        in_specs=[pl.BlockSpec(memory_space=pltpu.VMEM)] * 2,
        out_specs=pl.BlockSpec(memory_space=pltpu.VMEM),
        scratch_shapes=[
            pltpu.VMEM((n_kv, tokens, depth), jnp.bfloat16),
            pltpu.VMEM((n_kv, tokens, cols), jnp.bfloat16),
            pltpu.VMEM((n_tp, per, tokens, cols), jnp.bfloat16),
            dma((count,)), dma((n_kv,)), dma((n_kv,)), dma((n_tp, per)), dma((1,)),
        ],
        compiler_params=pltpu.CompilerParams(collective_id=1, has_side_effects=True),
        name="mix",
    )(y, weight)


def on_device(
    tokens,
    input_gain,
    gate_weight,
    value_weight,
    write_weight,
    read_weight,
    step_weight,
    conv_value,
    conv_write,
    conv_read,
    step_bias,
    decay_log,
    skip_gain,
    output_gain,
    out_weight,
    base_state,
    past_value,
    past_write,
    past_read,
    past_step,
    accepted,
):
    whole = lax.all_gather(tokens, "tp", axis=2, tiled=True)
    seq_local, proposals, width = whole.shape
    rows = whole.astype(jnp.float32)
    normed = (
        rows * lax.rsqrt(jnp.mean(rows * rows, axis=-1, keepdims=True) + EPSILON) * input_gain
    ).astype(jnp.bfloat16)
    flat = normed.reshape(seq_local * proposals, width)
    token_count = flat.shape[0]
    head_count = step_bias.shape[0]
    own_step = lax.dynamic_slice_in_dim(
        step_weight, lax.axis_index("tp") * head_count, head_count, 1
    )
    step_now = jnp.dot(flat, own_step, preferred_element_type=jnp.float32).astype(jnp.bfloat16)
    ranks, n_tp = lax.axis_size("kv"), lax.axis_size("tp")
    depth = gate_weight.shape[0]
    cut = [
        item.reshape(depth, ranks, item.shape[1] // ranks)
        for item in (gate_weight, value_weight, write_weight, read_weight)
    ]
    spans = [item.shape[2] for item in cut]
    wide = jnp.concatenate(cut[:2], axis=2).transpose(1, 0, 2)
    thin = jnp.concatenate(cut[2:], axis=2).transpose(1, 2, 0)
    half = width // n_tp
    own_features = lax.dynamic_slice_in_dim(flat, lax.axis_index("tp") * half, half, 1)
    returned = project(own_features, wide, thin, ranks, n_tp).transpose(1, 0, 2)
    pieces_out = []
    offset = 0
    for span in spans:
        pieces_out.append(returned[:, :, offset : offset + span].reshape(token_count, ranks * span))
        offset = offset + span
    gate_now, value_now, write_now, read_now = pieces_out
    shaped = [
        item.reshape(seq_local, proposals, item.shape[1])
        for item in (value_now, write_now, read_now, gate_now, step_now)
    ]
    stepper = jax.vmap(advance, in_axes=(0,) * 11 + (None,) * 7)
    normal_out, root_state, next_value, next_write, next_read = stepper(
        past_value,
        past_write,
        past_read,
        past_step,
        accepted,
        base_state,
        shaped[0],
        shaped[1],
        shaped[2],
        shaped[3],
        shaped[4],
        conv_value,
        conv_write,
        conv_read,
        step_bias,
        decay_log,
        skip_gain,
        output_gain,
    )
    flat_y = normal_out.reshape(token_count, -1)
    mixed = mix(flat_y, out_weight, ranks, n_tp)
    mixed = mixed.reshape(seq_local, proposals, mixed.shape[1])
    return (mixed, root_state, next_value, next_write, next_read, shaped[4])


def solution(mesh):
    return jax.shard_map(
        on_device,
        mesh=mesh,
        in_specs=(
            P("kv", None, "tp"),
            P(),
            P("kv", "tp"),
            P("kv", "tp"),
            P("kv", "tp"),
            P("kv", "tp"),
            P(),
            P(None, "tp"),
            P(None, "tp"),
            P(None, "tp"),
            P("tp"),
            P("tp"),
            P("tp"),
            P("tp"),
            P("tp", "kv"),
            P("kv", "tp", None, None),
            P("kv", None, "tp"),
            P("kv", None, "tp"),
            P("kv", None, "tp"),
            P("kv", None, "tp"),
            P("kv"),
        ),
        out_specs=(
            P("kv", None, "tp"),
            P("kv", "tp", None, None),
            P("kv", None, "tp"),
            P("kv", None, "tp"),
            P("kv", None, "tp"),
            P("kv", None, "tp"),
        ),
        check_vma=False,
    )
```

```python
import functools

import jax
import jax.numpy as jnp
from jax import lax
from jax.experimental import pallas as pl
from jax.experimental.pallas import tpu as pltpu
from jax.sharding import PartitionSpec as P

STATE_DIM = 128
CONV_W = 4


EPSILON = 1e-06


def causal_conv(rows, kernel):
    width = kernel.shape[0]
    count = rows.shape[0] - width + 1
    total = kernel[0] * rows[0:count]
    for offset in range(1, width):
        total = total + kernel[offset] * rows[offset : offset + count]
    return total


def advance(
    past_x,
    past_b,
    past_c,
    past_dt,
    taken,
    state_zero,
    value_now,
    write_now,
    read_now,
    gate_now,
    step_now,
    conv_value,
    conv_write,
    conv_read,
    step_bias,
    decay_log,
    skip_gain,
    output_gain,
):
    highest = lax.Precision.DEFAULT
    proposals = value_now.shape[0]
    head_count = step_bias.shape[0]
    group_count = write_now.shape[1] // STATE_DIM
    per_group = head_count // group_count
    head_width = value_now.shape[1] // head_count
    rate = jnp.exp(decay_log)
    prev_x = jax.nn.silu(causal_conv(past_x.astype(jnp.float32), conv_value)).reshape(
        proposals, head_count, head_width
    )
    prev_b = jax.nn.silu(causal_conv(past_b.astype(jnp.float32), conv_write)).reshape(
        proposals, group_count, STATE_DIM
    )
    prev_b = jnp.repeat(prev_b, per_group, axis=1)
    prev_dt = jax.nn.softplus(past_dt.astype(jnp.float32) + step_bias)
    live = (jnp.arange(proposals, dtype=jnp.int32) < taken)[:, None]
    prev_log = jnp.where(live, -rate * prev_dt, jnp.zeros_like(prev_dt))
    total_log = jnp.sum(prev_log, axis=0)
    tail_log = total_log - jnp.cumsum(prev_log, axis=0)
    weight_now = jnp.where(live, jnp.exp(tail_log) * prev_dt, jnp.zeros_like(prev_dt))
    root = jnp.exp(total_log)[:, None, None] * state_zero + jnp.einsum(
        "sh,shp,shn->hpn", weight_now, prev_x, prev_b, precision=highest
    )
    window_x = jnp.concatenate(
        [lax.dynamic_slice_in_dim(past_x, taken, CONV_W - 1, 0), value_now], axis=0
    )
    window_b = jnp.concatenate(
        [lax.dynamic_slice_in_dim(past_b, taken, CONV_W - 1, 0), write_now], axis=0
    )
    window_c = jnp.concatenate(
        [lax.dynamic_slice_in_dim(past_c, taken, CONV_W - 1, 0), read_now], axis=0
    )
    cur_x = jax.nn.silu(causal_conv(window_x.astype(jnp.float32), conv_value)).reshape(
        proposals, head_count, head_width
    )
    cur_b = jax.nn.silu(causal_conv(window_b.astype(jnp.float32), conv_write)).reshape(
        proposals, group_count, STATE_DIM
    )
    cur_c = jax.nn.silu(causal_conv(window_c.astype(jnp.float32), conv_read)).reshape(
        proposals, group_count, STATE_DIM
    )
    cur_b = jnp.repeat(cur_b, per_group, axis=1)
    cur_c = jnp.repeat(cur_c, per_group, axis=1)
    cur_dt = jax.nn.softplus(step_now.astype(jnp.float32) + step_bias)
    logs = jnp.cumsum(-rate * cur_dt, axis=0)
    carried = jnp.einsum("thn,hpn->thp", cur_c, root, precision=highest) * jnp.exp(logs)[:, :, None]
    lower = (jnp.arange(proposals)[:, None] >= jnp.arange(proposals)[None, :])[:, :, None]
    diff = logs[:, None, :] - logs[None, :, :]
    decay = jnp.where(
        lower, jnp.exp(jnp.where(lower, diff, jnp.zeros_like(diff))), jnp.zeros_like(diff)
    )
    scores = (
        jnp.einsum("thn,shn->tsh", cur_c, cur_b, precision=highest) * decay * cur_dt[None, :, :]
    )
    inner = jnp.einsum("tsh,shp->thp", scores, cur_x, precision=highest)
    mixed = carried + inner + skip_gain[None, :, None] * cur_x
    gated = mixed.reshape(proposals, -1) * jax.nn.silu(gate_now.astype(jnp.float32))
    grouped = gated.reshape(proposals, group_count, -1)
    grouped = grouped * lax.rsqrt(jnp.mean(grouped * grouped, axis=-1, keepdims=True) + EPSILON)
    result = (grouped.reshape(proposals, -1) * output_gain).astype(jnp.bfloat16)
    return (result, root, window_x, window_b, window_c)


MESH = pl.DeviceIdType.MESH


def near_split(count):
    low = max(d for d in range(1, count + 1) if count % d == 0 and d * d <= count)
    return count // low, low


def remote(src, dst, send, recv, kv, tp):
    return pltpu.make_async_remote_copy(
        src_ref=src,
        dst_ref=dst,
        send_sem=send,
        recv_sem=recv,
        device_id={"kv": kv, "tp": tp},
        device_id_type=MESH,
    )


class Gather:
    def __init__(self, own, slots, send, recv, n_kv):
        self.own, self.slots, self.send, self.recv = own, slots, send, recv
        self.far, self.near = near_split(n_kv)
        self.me, self.tp = lax.axis_index("kv"), lax.axis_index("tp")
        self.h, self.l = lax.div(self.me, self.near), lax.rem(self.me, self.near)
        self.copies = []

    def start(self, src, block, kv):
        copy = remote(
            src,
            self.slots.at[block],
            self.send.at[len(self.copies)],
            self.recv.at[block],
            kv,
            self.tp,
        )
        copy.start()
        self.copies.append(copy)

    def arrive(self, block):
        remote(
            self.own, self.slots.at[block], self.send.at[0], self.recv.at[block], self.me, self.tp
        ).wait_recv()

    def first(self):
        for step in range(1, self.far):
            self.start(self.own, self.me, lax.rem(self.h + step, self.far) * self.near + self.l)
        for step in range(1, self.near):
            self.start(self.own, self.me, self.h * self.near + lax.rem(self.l + step, self.near))

    def relay(self):
        for step in range(1, self.far):
            block = lax.rem(self.h + self.far - step, self.far) * self.near + self.l
            self.arrive(block)
            for side in range(1, self.near):
                self.start(
                    self.slots.at[block],
                    block,
                    self.h * self.near + lax.rem(self.l + side, self.near),
                )

    def finish(self):
        for side in range(1, self.near):
            l = lax.rem(self.l + self.near - side, self.near)
            for step in range(self.far):
                self.arrive(lax.rem(self.h + self.far - step, self.far) * self.near + l)

    def drain(self):
        for copy in self.copies:
            copy.wait_send()


def project_kernel(
    n_kv, n_tp, x_ref, wide_ref, thin_ref, out_ref,
    xs, wides, thins, mine, back,
    x_send, x_recv, tp_send, tp_recv, wide_send, wide_recv, thin_send, thin_recv,
    back_send, back_recv, local_sem,
):
    me, tp = lax.axis_index("kv"), lax.axis_index("tp")
    barrier = pltpu.get_barrier_semaphore()
    for step in range(1, n_kv):
        pl.semaphore_signal(
            barrier, inc=1, device_id={"kv": lax.rem(me + step, n_kv), "tp": tp}, device_id_type=MESH
        )
    for step in range(1, n_tp):
        pl.semaphore_signal(
            barrier, inc=1, device_id={"kv": me, "tp": lax.rem(tp + step, n_tp)}, device_id_type=MESH
        )
    own = [
        pltpu.make_async_copy(x_ref, xs.at[tp, me], local_sem.at[0]),
        pltpu.make_async_copy(wide_ref.at[me], wides.at[me], local_sem.at[1]),
        pltpu.make_async_copy(thin_ref.at[me], thins.at[me], local_sem.at[2]),
    ]
    for copy in own:
        copy.start()
    pl.semaphore_wait(barrier, n_kv - 1 + n_tp - 1)

    gather = Gather(x_ref, xs.at[tp], x_send, x_recv, n_kv)
    gather.first()
    sends = []

    def send_weights(lo, hi):
        for step in range(lo, hi):
            peer = lax.rem(me + step, n_kv)
            for src, dst, ss, rs in (
                (wide_ref, wides, wide_send, wide_recv),
                (thin_ref, thins, thin_send, thin_recv),
            ):
                copy = remote(src.at[peer], dst.at[me], ss.at[step - 1], rs.at[step - 1], peer, tp)
                copy.start()
                sends.append(copy)

    cut = 1 + n_kv // 4
    send_weights(1, cut)
    gather.relay()
    send_weights(cut, n_kv)
    gather.finish()
    for copy in own:
        copy.wait()
    shares = []
    for step in range(1, n_tp):
        copy = remote(
            xs.at[tp], xs.at[tp], tp_send.at[step - 1], tp_recv.at[step - 1],
            me, lax.rem(tp + step, n_tp),
        )
        copy.start()
        shares.append(copy)
    for copy in shares:
        copy.wait_recv()
    for copy in sends:
        copy.wait_recv()

    tokens = x_ref.shape[0]
    half = x_ref.shape[1]
    depth = wide_ref.shape[1]
    per = n_kv // n_tp
    wide_sum = None
    thin_sum = None
    for t in range(n_tp):
        rows = xs[t].reshape(n_kv * tokens, half)
        block = wides[t * per : (t + 1) * per].reshape(half, wide_ref.shape[2])
        term = jnp.dot(rows, block, preferred_element_type=jnp.float32)
        wide_sum = term if wide_sum is None else wide_sum + term
        for k in range(per):
            term = lax.dot_general(
                rows[:, k * depth : (k + 1) * depth],
                thins[t * per + k],
                (((1,), (1,)), ((), ())),
                preferred_element_type=jnp.float32,
            )
            thin_sum = term if thin_sum is None else thin_sum + term
    wide_cols = wide_ref.shape[2]
    cols = mine.shape[2]
    mine[:, :, 0:wide_cols] = wide_sum.astype(jnp.bfloat16).reshape(n_kv, tokens, wide_cols)
    mine[:, :, wide_cols:cols] = thin_sum.astype(jnp.bfloat16).reshape(
        n_kv, tokens, cols - wide_cols
    )
    returns = []
    for step in range(1, n_kv):
        peer = lax.rem(me + step, n_kv)
        copy = remote(
            mine.at[peer], back.at[me], back_send.at[step - 1], back_recv.at[step - 1], peer, tp
        )
        copy.start()
        returns.append(copy)
    out_ref[me] = mine[me]
    gather.drain()
    for copy in shares + sends:
        copy.wait_send()
    for step, copy in enumerate(returns, 1):
        copy.wait_recv()
        source = lax.rem(me + n_kv - step, n_kv)
        out_ref[source] = back[source]
    for copy in returns:
        copy.wait_send()


def project(x, wide, thin, n_kv, n_tp):
    tokens, half = x.shape
    cols = wide.shape[2] + thin.shape[1]
    dma = pltpu.SemaphoreType.DMA
    far, near = near_split(n_kv)
    count = far - 1 + (near - 1) * far
    peers = (max(n_kv - 1, 1),)
    return pl.pallas_call(
        functools.partial(project_kernel, n_kv, n_tp),
        out_shape=jax.ShapeDtypeStruct((n_kv, tokens, cols), jnp.bfloat16),
        in_specs=[pl.BlockSpec(memory_space=pltpu.VMEM)] * 3,
        out_specs=pl.BlockSpec(memory_space=pltpu.VMEM),
        scratch_shapes=[
            pltpu.VMEM((n_tp, n_kv, tokens, half), jnp.bfloat16),
            pltpu.VMEM(wide.shape, jnp.bfloat16),
            pltpu.VMEM(thin.shape, jnp.bfloat16),
            pltpu.VMEM((n_kv, tokens, cols), jnp.bfloat16),
            pltpu.VMEM((n_kv, tokens, cols), jnp.bfloat16),
            dma((count,)), dma((n_kv,)), dma((max(n_tp - 1, 1),)), dma((max(n_tp - 1, 1),)),
            dma(peers), dma(peers), dma(peers), dma(peers), dma(peers), dma(peers), dma((3,)),
        ],
        compiler_params=pltpu.CompilerParams(collective_id=0, has_side_effects=True),
        name="project",
    )(x, wide, thin)


def mix_kernel(
    n_kv, n_tp, y_ref, w_ref, out_ref,
    ys, mine, parts, y_send, y_recv, part_send, part_recv, local_sem,
):
    me, tp = lax.axis_index("kv"), lax.axis_index("tp")
    total = n_kv * n_tp
    flat = me * n_tp + tp
    barrier = pltpu.get_barrier_semaphore()

    def greet(step, carry):
        other = lax.rem(flat + step, total)
        pl.semaphore_signal(
            barrier,
            inc=1,
            device_id={"kv": lax.div(other, n_tp), "tp": lax.rem(other, n_tp)},
            device_id_type=MESH,
        )
        return carry

    lax.fori_loop(1, total, greet, 0)
    own = pltpu.make_async_copy(y_ref, ys.at[me], local_sem.at[0])
    own.start()
    pl.semaphore_wait(barrier, total - 1)
    gather = Gather(y_ref, ys, y_send, y_recv, n_kv)
    gather.first()
    gather.relay()
    own.wait()
    gather.finish()

    tokens, cols = y_ref.shape[0], w_ref.shape[1]
    product = jnp.dot(
        ys[...].reshape(n_kv * tokens, y_ref.shape[1]),
        w_ref[...],
        preferred_element_type=jnp.float32,
    )
    mine[...] = product.astype(jnp.bfloat16).reshape(n_kv, tokens, cols)
    per = n_kv // n_tp
    side, place = lax.div(me, per), lax.rem(me, per)

    def part(step):
        return remote(
            mine.at[lax.rem(me + step, n_kv)],
            parts.at[tp, place],
            part_send.at[step],
            part_recv.at[tp, place],
            lax.rem(me + step, n_kv),
            side,
        )

    for step in range(1, n_kv):
        part(step).start()

    @pl.when(side != tp)
    def _():
        part(0).start()

    @pl.when(side == tp)
    def _():
        parts[tp, place] = mine[me]

    gather.drain()
    for t in range(n_tp):
        for k in range(per):
            incoming = remote(
                mine.at[0], parts.at[t, k], part_send.at[0], part_recv.at[t, k], me, tp
            )

            @pl.when(jnp.logical_or(t != tp, tp * per + k != me))
            def _():
                incoming.wait_recv()

    for k in range(per):
        value = parts[0, k].astype(jnp.float32)
        for t in range(1, n_tp):
            value = value + parts[t, k].astype(jnp.float32)
        out_ref[:, k * cols : (k + 1) * cols] = value.astype(jnp.bfloat16)
    for step in range(1, n_kv):
        part(step).wait_send()

    @pl.when(side != tp)
    def _():
        part(0).wait_send()


def mix(y, weight, n_kv, n_tp):
    tokens, depth = y.shape
    cols = weight.shape[1]
    dma = pltpu.SemaphoreType.DMA
    far, near = near_split(n_kv)
    count = far - 1 + (near - 1) * far
    per = n_kv // n_tp
    return pl.pallas_call(
        functools.partial(mix_kernel, n_kv, n_tp),
        out_shape=jax.ShapeDtypeStruct((tokens, per * cols), jnp.bfloat16),
        in_specs=[pl.BlockSpec(memory_space=pltpu.VMEM)] * 2,
        out_specs=pl.BlockSpec(memory_space=pltpu.VMEM),
        scratch_shapes=[
            pltpu.VMEM((n_kv, tokens, depth), jnp.bfloat16),
            pltpu.VMEM((n_kv, tokens, cols), jnp.bfloat16),
            pltpu.VMEM((n_tp, per, tokens, cols), jnp.bfloat16),
            dma((count,)), dma((n_kv,)), dma((n_kv,)), dma((n_tp, per)), dma((1,)),
        ],
        compiler_params=pltpu.CompilerParams(collective_id=1, has_side_effects=True),
        name="mix",
    )(y, weight)


def on_device(
    tokens,
    input_gain,
    gate_weight,
    value_weight,
    write_weight,
    read_weight,
    step_weight,
    conv_value,
    conv_write,
    conv_read,
    step_bias,
    decay_log,
    skip_gain,
    output_gain,
    out_weight,
    base_state,
    past_value,
    past_write,
    past_read,
    past_step,
    accepted,
):
    whole = lax.all_gather(tokens, "tp", axis=2, tiled=True)
    seq_local, proposals, width = whole.shape
    rows = whole.astype(jnp.float32)
    normed = (
        rows * lax.rsqrt(jnp.mean(rows * rows, axis=-1, keepdims=True) + EPSILON) * input_gain
    ).astype(jnp.bfloat16)
    flat = normed.reshape(seq_local * proposals, width)
    token_count = flat.shape[0]
    head_count = step_bias.shape[0]
    own_step = lax.dynamic_slice_in_dim(
        step_weight, lax.axis_index("tp") * head_count, head_count, 1
    )
    step_now = jnp.dot(flat, own_step, preferred_element_type=jnp.float32).astype(jnp.bfloat16)
    ranks, n_tp = lax.axis_size("kv"), lax.axis_size("tp")
    depth = gate_weight.shape[0]
    cut = [
        item.reshape(depth, ranks, item.shape[1] // ranks)
        for item in (gate_weight, value_weight, write_weight, read_weight)
    ]
    spans = [item.shape[2] for item in cut]
    wide = jnp.concatenate(cut[:2], axis=2).transpose(1, 0, 2)
    thin = jnp.concatenate(cut[2:], axis=2).transpose(1, 2, 0)
    half = width // n_tp
    own_features = lax.dynamic_slice_in_dim(flat, lax.axis_index("tp") * half, half, 1)
    returned = project(own_features, wide, thin, ranks, n_tp).transpose(1, 0, 2)
    pieces_out = []
    offset = 0
    for span in spans:
        pieces_out.append(returned[:, :, offset : offset + span].reshape(token_count, ranks * span))
        offset = offset + span
    gate_now, value_now, write_now, read_now = pieces_out
    shaped = [
        item.reshape(seq_local, proposals, item.shape[1])
        for item in (value_now, write_now, read_now, gate_now, step_now)
    ]
    stepper = jax.vmap(advance, in_axes=(0,) * 11 + (None,) * 7)
    normal_out, root_state, next_value, next_write, next_read = stepper(
        past_value,
        past_write,
        past_read,
        past_step,
        accepted,
        base_state,
        shaped[0],
        shaped[1],
        shaped[2],
        shaped[3],
        shaped[4],
        conv_value,
        conv_write,
        conv_read,
        step_bias,
        decay_log,
        skip_gain,
        output_gain,
    )
    flat_y = normal_out.reshape(token_count, -1)
    mixed = mix(flat_y, out_weight, ranks, n_tp)
    mixed = mixed.reshape(seq_local, proposals, mixed.shape[1])
    return (mixed, root_state, next_value, next_write, next_read, shaped[4])


def solution(mesh):
    return jax.shard_map(
        on_device,
        mesh=mesh,
        in_specs=(
            P("kv", None, "tp"),
            P(),
            P("kv", "tp"),
            P("kv", "tp"),
            P("kv", "tp"),
            P("kv", "tp"),
            P(),
            P(None, "tp"),
            P(None, "tp"),
            P(None, "tp"),
            P("tp"),
            P("tp"),
            P("tp"),
            P("tp"),
            P("tp", "kv"),
            P("kv", "tp", None, None),
            P("kv", None, "tp"),
            P("kv", None, "tp"),
            P("kv", None, "tp"),
            P("kv", None, "tp"),
            P("kv"),
        ),
        out_specs=(
            P("kv", None, "tp"),
            P("kv", "tp", None, None),
            P("kv", None, "tp"),
            P("kv", None, "tp"),
            P("kv", None, "tp"),
            P("kv", None, "tp"),
        ),
        check_vma=False,
    )
```
